32 devices in a mesh: sp: 8 (over z, x), tp: 4 (over y, core).
Axes of the slice: x: 2, y: 2, z: 4, core: 2. Of those that a mesh axis runs over, the one named last changes fastest.
Arguments:
- x_res: bfloat16 [2048, 2048], P(('sp', 'tp')), may hold values from -6 to 6
- q_a: bfloat16 [2048, 1024], P('sp', 'tp'), may hold values from -48 to 48
- k_a: bfloat16 [2048, 256], P('sp', 'tp'), may hold values from -48 to 48
- v_a: bfloat16 [2048, 256], P('sp', 'tp'), may hold values from -6 to 6
- q_b: bfloat16 [2048, 1024], P('sp', 'tp'), may hold values from -48 to 48
- k_b: bfloat16 [2048, 512], P('sp', 'tp'), may hold values from -48 to 48
- v_b: bfloat16 [2048, 512], P('sp', 'tp'), may hold values from -6 to 6
- gain_qa: float32 [64], replicated, may hold values from 1.2 to 6
- gain_ka: float32 [64], replicated, may hold values from 1.2 to 6
- gain_qb: float32 [128], replicated, may hold values from 1.2 to 6
- gain_kb: float32 [128], replicated, may hold values from 1.2 to 6
- w_out_a: bfloat16 [1024, 2048], P('tp'), may hold values from -0.125 to 0.125
- w_out_b: bfloat16 [1024, 2048], P('tp'), may hold values from -0.125 to 0.125
- gain_mid: float32 [2048], replicated, may hold values from 0.1 to 1.9
- w_gate: bfloat16 [2048, 3072], P('sp', 'tp'), may hold values from -0.125 to 0.125
- w_up: bfloat16 [2048, 3072], P('sp', 'tp'), may hold values from -0.125 to 0.125
- conv_gate: float32 [3, 3072], P(None, 'tp'), may hold values from -3.5 to 3.5
- conv_up: float32 [3, 3072], P(None, 'tp'), may hold values from -3.5 to 3.5
- w_down: bfloat16 [3072, 2048], P('tp', 'sp'), may hold values from -0.109375 to 0.109375
Outputs:
- layer_out: bfloat16 [2048, 2048], P(('sp', 'tp'))
The draws below stay inside these ranges and needn't reach their ends.
All inputs are finite; a program needn't handle non-finite values.
Results may differ from the reference program's by a relative error of at most 0.014.
The reference program's roundings to bfloat16 on the way (of `qa_n`, `ka_n`, `qb_n`, `kb_n`, `normed`, `gate_pre`, `up_pre` and `hidden`) count: a program that leaves them out, or rounds other values in their place, can miss the bound.
Values may be sent and summed in bfloat16 or wider, within the bound.
A program may use at most 128 MiB of HBM per device.

```python
import jax
import jax.numpy as jnp
from jax import lax

D = 2048
FF = 3072
HQA = 16
HKVA = 4
DHA = 64
HQB = 8
HKVB = 4
DHB = 128
TOKENS = 2048
N_TP = 4


def drawn_keys(key, heads, head_size, salt):
    base = jax.random.fold_in(key, salt)
    streams = jax.random.split(base, 1)
    keys = jax.random.truncated_normal(streams[0], -4.0, 4.0, (TOKENS, heads, head_size), jnp.float32)
    return keys


def drawn_queries(key, heads, head_size, salt):
    queries = jax.random.truncated_normal(jax.random.fold_in(key, salt + 1), -4.0, 4.0, (TOKENS, heads, head_size), jnp.float32)
    return queries.reshape(TOKENS, heads * head_size).astype(jnp.bfloat16)


def drawn_gain(key, head_size, salt):
    gains = jax.random.uniform(jax.random.fold_in(key, salt), (head_size,), jnp.float32, 1.2, 2.4)
    return gains


def draw_q_a(key, part):
    return drawn_queries(key, HQA, DHA, 11)


def draw_k_a(key, part):
    keys = drawn_keys(key, HKVA, DHA, 11)
    return keys.reshape(TOKENS, HKVA * DHA).astype(jnp.bfloat16)


def draw_q_b(key, part):
    return drawn_queries(key, HQB, DHB, 21)


def draw_k_b(key, part):
    keys = drawn_keys(key, HKVB, DHB, 21)
    return keys.reshape(TOKENS, HKVB * DHB).astype(jnp.bfloat16)


def draw_gain_qa(key, part):
    return drawn_gain(key, DHA, 31)


def draw_gain_ka(key, part):
    return drawn_gain(key, DHA, 32)


def draw_gain_qb(key, part):
    return drawn_gain(key, DHB, 33)


def draw_gain_kb(key, part):
    return drawn_gain(key, DHB, 34)


def steps_of(rng, extent, pieces, low, top_value):
    def one(axis_at, blocks):
        heights = jax.random.uniform(jax.random.fold_in(jax.random.fold_in(rng, 6), axis_at), (blocks,), jnp.float32, low / len(pieces), top_value / len(pieces))
        return jnp.repeat(jnp.exp(heights), extent[axis_at] // blocks).reshape((-1,) + (1,) * (len(extent) - axis_at - 1))

    level = one(*pieces[0])
    for cut in pieces[1:]:
        level = level * one(*cut)
    return level


def noise(rng, extent, deviation, bound, cuts=(), held_as=jnp.bfloat16):
    level = steps_of(rng, extent, cuts, -0.22, 0.18) if cuts else 1.0
    values = jax.random.normal(rng, extent, jnp.float32) * deviation * level
    return jnp.minimum(jnp.maximum(values, -bound), bound).astype(held_as)


def setup_inputs(seed: int = 0) -> dict:
    streams_of = jax.random.split(jax.random.key(seed), 20)
    return {
        "x_res": noise(streams_of[0], (TOKENS, D), 1.0, 6.0, ((0, 32),)),
        "q_a": draw_q_a(jax.random.fold_in(streams_of[19], 71), 0),
        "k_a": draw_k_a(jax.random.fold_in(streams_of[19], 71), 0),
        "v_a": noise(streams_of[3], (TOKENS, HKVA * DHA), 1.0, 6.0, ((0, 8), (1, 4))),
        "q_b": draw_q_b(jax.random.fold_in(streams_of[19], 71), 0),
        "k_b": draw_k_b(jax.random.fold_in(streams_of[19], 71), 0),
        "v_b": noise(streams_of[6], (TOKENS, HKVB * DHB), 1.0, 6.0, ((0, 8), (1, 4))),
        "gain_qa": draw_gain_qa(jax.random.fold_in(streams_of[19], 71), 0),
        "gain_ka": draw_gain_ka(jax.random.fold_in(streams_of[19], 71), 0),
        "gain_qb": draw_gain_qb(jax.random.fold_in(streams_of[19], 71), 0),
        "gain_kb": draw_gain_kb(jax.random.fold_in(streams_of[19], 71), 0),
        "w_out_a": noise(streams_of[11], (HQA * DHA, D), (HQA * DHA + HQB * DHB) ** -0.5, 0.125, ((0, 4),)),
        "w_out_b": noise(streams_of[12], (HQB * DHB, D), (HQA * DHA + HQB * DHB) ** -0.5, 0.125, ((0, 4),)),
        "gain_mid": jnp.clip(1.0 + 0.18 * jax.random.normal(streams_of[13], (D,), jnp.float32), 0.1, 1.9),
        "w_gate": noise(streams_of[14], (D, FF), D ** -0.5, 0.125, ((0, 8), (1, 4))),
        "w_up": noise(streams_of[15], (D, FF), D ** -0.5, 0.125, ((0, 8), (1, 4))),
        "conv_gate": noise(streams_of[16], (3, FF), 3 ** -0.5, 3.5, ((1, 4),), jnp.float32),
        "conv_up": noise(streams_of[17], (3, FF), 3 ** -0.5, 3.5, ((1, 4),), jnp.float32),
        "w_down": noise(streams_of[18], (FF, D), FF ** -0.5, 0.109375, ((0, 4), (1, 8))),
    }


norm_eps = 1e-06
rope_theta = 10000.0

def rotary_angles(positions, head_size):
    half = head_size // 2
    inverse = jnp.power(jnp.float32(rope_theta), -jnp.arange(0, half, 2, dtype=jnp.float32) / half)
    grid_row = (positions // 64).astype(jnp.float32)[:, None] * inverse[None, :]
    grid_col = (positions % 64).astype(jnp.float32)[:, None] * inverse[None, :]
    angles = jnp.concatenate([grid_row, grid_row, grid_col, grid_col], axis=-1)
    return (jnp.cos(angles), jnp.sin(angles))

def rotate_half(values):
    first, second = jnp.split(values, 2, axis=-1)
    return jnp.concatenate([-second, first], axis=-1)

def prepare(raw, gain, head_size, positions):
    count = raw.shape[0]
    heads = raw.shape[1] // head_size
    values = raw.astype(jnp.float32).reshape(count, heads, head_size)
    values = values * lax.rsqrt(lax.optimization_barrier(jnp.mean(values * values, axis=-1, keepdims=True)) + norm_eps)
    values = values * gain.astype(jnp.float32)
    cosine, sine = rotary_angles(positions, head_size)
    row_part, col_part = jnp.split(values, 2, axis=-1)
    turned = jnp.concatenate([rotate_half(row_part), rotate_half(col_part)], axis=-1)
    values = values * cosine[:, None, :] + turned * sine[:, None, :]
    return values.astype(jnp.bfloat16)

def attention_group(queries, keys, values, head_size):
    count = queries.shape[0]
    kv_heads = keys.shape[1]
    groups = queries.shape[1] // kv_heads
    block = 256 if count % 256 == 0 else 64
    blocked = queries.reshape(count // block, block, kv_heads, groups, head_size)
    keys_f = keys.astype(jnp.float32)
    values_f = values.astype(jnp.float32)
    scale = jnp.float32(head_size ** (-0.5))

    def one_block(query_block):
        scores = jnp.einsum('qkgd,skd->kgqs', query_block.astype(jnp.float32), keys_f) * scale
        top = lax.optimization_barrier(jnp.max(scores, axis=-1, keepdims=True))
        expd = jnp.exp(scores - top)
        totals = lax.optimization_barrier(jnp.sum(expd, axis=-1))
        weights = expd.astype(jnp.bfloat16).astype(jnp.float32)
        summed = jnp.einsum('kgqs,skd->kgqd', weights, values_f) / totals[..., None]
        return jnp.transpose(summed, (2, 0, 1, 3)).reshape(block, kv_heads * groups * head_size).astype(jnp.bfloat16)
    result = lax.map(one_block, blocked)
    return result.reshape(count, kv_heads * groups * head_size)

def reference(x_res, q_a, k_a, v_a, q_b, k_b, v_b, gain_qa, gain_ka, gain_qb, gain_kb, w_out_a, w_out_b, gain_mid, w_gate, w_up, conv_gate, conv_up, w_down):
    count = x_res.shape[0]
    positions = jnp.arange(count, dtype=jnp.int32)
    qa_n = prepare(q_a, gain_qa, DHA, positions)
    ka_n = prepare(k_a, gain_ka, DHA, positions)
    qb_n = prepare(q_b, gain_qb, DHB, positions)
    kb_n = prepare(k_b, gain_kb, DHB, positions)
    va_h = v_a.reshape(count, HKVA, DHA)
    vb_h = v_b.reshape(count, HKVB, DHB)
    attn_a = attention_group(qa_n, ka_n, va_h, DHA)
    attn_b = attention_group(qb_n, kb_n, vb_h, DHB)
    width_a = HQA * DHA // N_TP
    width_b = HQB * DHB // N_TP
    projected = jnp.zeros((count, D), jnp.float32)
    for block in range(N_TP):
        partial_value = jnp.dot(attn_a[:, block * width_a:(block + 1) * width_a], w_out_a[block * width_a:(block + 1) * width_a], preferred_element_type=jnp.float32)
        partial_value = partial_value + jnp.dot(attn_b[:, block * width_b:(block + 1) * width_b], w_out_b[block * width_b:(block + 1) * width_b], preferred_element_type=jnp.float32)
        projected = projected + partial_value.astype(jnp.bfloat16).astype(jnp.float32)
    mid = x_res.astype(jnp.float32) + projected
    normed = mid * lax.rsqrt(lax.optimization_barrier(jnp.mean(mid * mid, axis=-1, keepdims=True)) + norm_eps)
    normed = (normed * gain_mid.astype(jnp.float32)).astype(jnp.bfloat16)
    gate_pre = jnp.dot(normed, w_gate, preferred_element_type=jnp.float32).astype(jnp.bfloat16)
    up_pre = jnp.dot(normed, w_up, preferred_element_type=jnp.float32).astype(jnp.bfloat16)

    def convolve(projected_rows, taps):
        padded = jnp.pad(projected_rows.astype(jnp.float32), ((1, 1), (0, 0)))
        taps = taps.astype(jnp.float32)
        return padded[:-2] * taps[0] + padded[1:-1] * taps[1] + padded[2:] * taps[2]
    gate_conv = convolve(gate_pre, conv_gate)
    up_conv = convolve(up_pre, conv_up)
    hidden = (jax.nn.silu(gate_conv) * up_conv).astype(jnp.bfloat16)
    width_f = FF // N_TP
    down = jnp.zeros((count, D), jnp.float32)
    for block in range(N_TP):
        partial_value = jnp.dot(hidden[:, block * width_f:(block + 1) * width_f], w_down[block * width_f:(block + 1) * width_f], preferred_element_type=jnp.float32)
        down = down + partial_value.astype(jnp.bfloat16).astype(jnp.float32)
    return (mid + down).astype(jnp.bfloat16)
```

```python
import functools

import jax
import jax.numpy as jnp
from jax import lax
from jax.experimental import pallas as pl
from jax.experimental.pallas import tpu as pltpu
from jax.sharding import PartitionSpec as P

DHA = 64
DHB = 128

norm_eps = 1e-06
rope_theta = 10000.0
F32 = jnp.float32
BF16 = jnp.bfloat16
MESH = pl.DeviceIdType.MESH
PIECES = 2


def rotary_angles(positions, head_size):
    half = head_size // 2
    inverse = jnp.power(jnp.float32(rope_theta), -jnp.arange(0, half, 2, dtype=jnp.float32) / half)
    grid_row = (positions // 64).astype(jnp.float32)[:, None] * inverse[None, :]
    grid_col = (positions % 64).astype(jnp.float32)[:, None] * inverse[None, :]
    return jnp.concatenate([grid_row, grid_row, grid_col, grid_col], axis=-1)


def block_mean(width, head):
    i = lax.broadcasted_iota(jnp.int32, (width, width), 0)
    j = lax.broadcasted_iota(jnp.int32, (width, width), 1)
    return jnp.where(lax.div(i, head) == lax.div(j, head), F32(1.0 / head), F32(0.0))


def block_turn(width, head):
    quarter = head // 4
    i = lax.broadcasted_iota(jnp.int32, (width, width), 0)
    j = lax.broadcasted_iota(jnp.int32, (width, width), 1)
    first = lax.rem(j, 2 * quarter) < quarter
    return jnp.where(
        first & (i == j + quarter),
        F32(-1.0),
        jnp.where(jnp.logical_not(first) & (i == j - quarter), F32(1.0), F32(0.0)),
    )


def exact_dot(a, b):
    return jnp.dot(a, b, precision=lax.Precision.HIGHEST, preferred_element_type=F32)


def prepared(raw, gain, angle_cos, angle_sin, head):
    width = raw.shape[1]
    values = raw.astype(F32)
    values = values * lax.rsqrt(exact_dot(values * values, block_mean(width, head)) + norm_eps)
    values = values * gain
    turned = exact_dot(values, block_turn(width, head))
    return (values * angle_cos + turned * angle_sin).astype(BF16)


def kernel(
    n, tp_n,
    x_ref, qa_ref, ka_ref, va_ref, qb_ref, kb_ref, vb_ref,
    gqa_ref, gka_ref, gqb_ref, gkb_ref,
    cosa_ref, sina_ref, cosb_ref, sinb_ref,
    woa_hbm, wob_hbm, gmid_ref, wg_hbm, wu_hbm, cg_ref, cu_ref, wd_hbm,
    out_ref,
    kv, qas, qbs, m_a, l_a, acc_a, m_b, l_b, acc_b,
    woa, wob, wg, wu, wdr, wdl,
    attn, part, rs_in, mid, nrm, acc_g, acc_u, joined, halo_lo, halo_hi, hidden, acc_d, part2, rs2_in,
    loc_sem, kv_send, kv_recv, w_send, w_recv, d_send, d_recv,
    rs_send, rs_recv, ag_send, ag_recv, h_send, h_recv, r2_send, r2_recv,
):
    sp = lax.axis_index("sp")
    tp = lax.axis_index("tp")
    rows = qa_ref.shape[0]
    own = x_ref.shape[0]
    half = n // 2

    odd = lax.rem(sp, 2)
    pos = (1 - odd) * lax.div(sp, 2) + odd * (n - 1 - lax.div(sp, 2))

    def at(p):
        p = lax.rem(p + 2 * n, n)
        back = lax.div(p, half)
        return (1 - back) * 2 * p + back * (2 * (n - 1 - p) + 1)

    right, left = at(pos + 1), at(pos - 1)
    above, below = lax.rem(sp + 1, n), lax.rem(sp + n - 1, n)

    barrier = pltpu.get_barrier_semaphore()
    for other in (right, left, above, below):
        pl.semaphore_signal(barrier, inc=1, device_id={"sp": other}, device_id_type=MESH)
    for d in range(1, tp_n):
        pl.semaphore_signal(
            barrier, inc=1, device_id={"tp": lax.rem(tp + d, tp_n)}, device_id_type=MESH
        )

    locals_ = [
        pltpu.make_async_copy(woa_hbm, woa, loc_sem.at[0]),
        pltpu.make_async_copy(wob_hbm, wob, loc_sem.at[1]),
        pltpu.make_async_copy(wg_hbm, wg.at[0], loc_sem.at[2]),
        pltpu.make_async_copy(wu_hbm, wu.at[0], loc_sem.at[3]),
        pltpu.make_async_copy(wd_hbm.at[pl.ds(0, wdr.shape[1])], wdr.at[0], loc_sem.at[4]),
        pltpu.make_async_copy(
            wd_hbm.at[pl.ds(wdr.shape[1], wdr.shape[1])], wdl.at[0], loc_sem.at[5]
        ),
    ]
    for copy in locals_:
        copy.start()

    def remote(src, dst, send, recv, **where):
        return pltpu.make_async_remote_copy(
            src_ref=src, dst_ref=dst, send_sem=send, recv_sem=recv,
            device_id=where, device_id_type=MESH,
        )

    ca, sa, cb, sb = cosa_ref[...], sina_ref[...], cosb_ref[...], sinb_ref[...]
    wka, wkb = ka_ref.shape[1], kb_ref.shape[1]

    def wide(table, width):
        if width <= table.shape[1]:
            return table[:, :width]
        return jnp.concatenate([table] * (width // table.shape[1]), axis=1)

    def gains(ref, width):
        g = ref[...]
        count = width // g.shape[1]
        return g if count == 1 else jnp.concatenate([g] * count, axis=1)

    keys_a = prepared(ka_ref[...], gains(gka_ref, wka), wide(ca, wka), wide(sa, wka), DHA)
    keys_b = prepared(kb_ref[...], gains(gkb_ref, wkb), wide(cb, wkb), wide(sb, wkb), DHB)
    kv[0, :, :wkb] = keys_b
    kv[0, :, wkb:2 * wkb] = vb_ref[...]
    kv[0, :, 2 * wkb:] = jnp.concatenate([keys_a, va_ref[...]], axis=1)
    pl.semaphore_wait(barrier, 4 + tp_n - 1)

    def kv_r(s):
        return remote(kv.at[s - 1], kv.at[s], kv_send.at[s], kv_recv.at[s], sp=right)

    def kv_l(s):
        source = lax.rem(n - s + 1, n)
        return remote(kv.at[source], kv.at[n - s], kv_send.at[n - s], kv_recv.at[n - s], sp=left)

    wrows = wg.shape[1] // PIECES
    drows = wdr.shape[1] // PIECES

    def w_copy(s, p, direction):
        buf, to = (wg, right) if direction == 0 else (wu, left)
        cut = pl.ds(p * wrows, wrows)
        return remote(
            buf.at[s - 1, cut], buf.at[s, cut],
            w_send.at[direction, p, s], w_recv.at[direction, p, s], sp=to,
        )

    def d_copy(s, p, direction):
        buf, to = (wdr, right) if direction == 0 else (wdl, left)
        cut = pl.ds(p * drows, drows)
        return remote(
            buf.at[s - 1, cut], buf.at[s, cut],
            d_send.at[direction, p, s], d_recv.at[direction, p, s], sp=to,
        )

    def tick(copy, s, following=None):
        for p in range(PIECES):
            for direction in range(2):
                copy(s, p, direction).wait_recv()
                if following is None:
                    copy(s + 1, p, direction).start()
                elif following != "end":
                    following(1, p, direction).start()

    kv_r(1).start()
    kv_l(1).start()

    heads_a = qa_ref.shape[1] // DHA
    heads_b = qb_ref.shape[1] // DHB
    qa = prepared(
        qa_ref[...], gains(gqa_ref, heads_a * DHA), wide(ca, heads_a * DHA),
        wide(sa, heads_a * DHA), DHA,
    )
    qb = prepared(
        qb_ref[...], gains(gqb_ref, heads_b * DHB), wide(cb, heads_b * DHB),
        wide(sb, heads_b * DHB), DHB,
    )
    for h in range(heads_a):
        qas[h] = qa[:, h * DHA:(h + 1) * DHA]
    for h in range(heads_b):
        qbs[h] = qb[:, h * DHB:(h + 1) * DHB]
    for ref, low in ((m_a, -1e30), (m_b, -1e30), (l_a, 0.0), (l_b, 0.0), (acc_a, 0.0), (acc_b, 0.0)):
        ref[...] = jnp.full(ref.shape, low, F32)

    def attend_one(queries, key_rows, value_rows, m, l, acc, h):
        scale = F32(queries.shape[2] ** (-0.5))
        scores = lax.dot_general(
            queries[h], key_rows, (((1,), (1,)), ((), ())), preferred_element_type=F32
        ) * scale
        before = m[h]
        highest = jnp.maximum(before, jnp.max(scores, axis=-1, keepdims=True))
        factor = jnp.exp(before - highest)
        expd = jnp.exp(scores - highest)
        l[h] = l[h] * factor + jnp.sum(expd, axis=-1, keepdims=True)
        acc[h] = acc[h] * factor + jnp.dot(
            expd.astype(BF16), value_rows, preferred_element_type=F32
        )
        m[h] = highest

    def attend(slot):
        for h in range(heads_b):
            attend_one(qbs, kv[slot, :, :wkb], kv[slot, :, wkb:2 * wkb], m_b, l_b, acc_b, h)
        pair = kv[slot, :, 2 * wkb:]
        for h in range(heads_a):
            attend_one(qas, pair[:, :wka], pair[:, wka:], m_a, l_a, acc_a, h)

    attend(0)

    def kv_step(s, carry):
        kv_r(s).wait_recv()
        kv_r(s + 1).start()
        kv_l(s).wait_recv()

        @pl.when(s < half - 1)
        def _():
            kv_l(s + 1).start()

        @pl.when(s == half - 1)
        def _():
            for p in range(PIECES):
                for direction in range(2):
                    w_copy(1, p, direction).start()

        def one(i, inner):
            attend((1 - i) * s + i * (n - s))
            return inner

        lax.fori_loop(0, 2, one, 0)
        return carry

    for copy in locals_:
        copy.wait()
    lax.fori_loop(1, half, kv_step, 0)
    kv_r(half).wait_recv()
    attend(half)

    for h in range(heads_a):
        attn[:, h * DHA:(h + 1) * DHA] = (acc_a[h] / l_a[h]).astype(BF16)
    width_a = heads_a * DHA
    for h in range(heads_b):
        attn[:, width_a + h * DHB:width_a + (h + 1) * DHB] = (acc_b[h] / l_b[h]).astype(BF16)

    def rs_copy(d):
        to = lax.rem(tp + d, tp_n)
        return remote(
            part.at[pl.ds(pl.multiple_of(to * own, own), own)], rs_in.at[d - 1],
            rs_send.at[d - 1], rs_recv.at[d - 1], tp=to,
        )

    for i in range(tp_n):
        d = tp_n - 1 - i
        at_rows = pl.ds(pl.multiple_of(lax.rem(tp + d, tp_n) * own, own), own)
        block = attn[at_rows, :]
        part[at_rows, :] = (
            jnp.dot(block[:, :width_a], woa[...], preferred_element_type=F32)
            + jnp.dot(block[:, width_a:], wob[...], preferred_element_type=F32)
        ).astype(BF16)
        if d > 0:
            rs_copy(d).start()

    early = max(1, n // 8)

    def w_tick(s, carry):
        tick(w_copy, s)
        return carry

    lax.fori_loop(1, early + 1, w_tick, 0)

    mine = pl.ds(pl.multiple_of(tp * own, own), own)
    total = part[mine, :].astype(F32)
    for d in range(1, tp_n):
        rs_copy(d).wait_recv()
        total = total + rs_in[d - 1].astype(F32)
    middle = x_ref[...].astype(F32) + total
    mid[...] = middle
    normed = middle * lax.rsqrt(jnp.mean(middle * middle, axis=-1, keepdims=True) + norm_eps)
    nrm[mine, :] = (normed * gmid_ref[...]).astype(BF16)

    def ag_copy(d):
        return remote(
            nrm.at[mine], nrm.at[mine], ag_send.at[d - 1], ag_recv.at[d - 1],
            tp=lax.rem(tp + d, tp_n),
        )

    for d in range(1, tp_n):
        ag_copy(d).start()
    lax.fori_loop(early + 1, 2 * early + 1, w_tick, 0)
    for d in range(1, tp_n):
        ag_copy(d).wait_recv()

    chunk = wg.shape[1]

    def columns(p, width):
        return pl.ds(pl.multiple_of(at(p) * width, width), width)

    def gate_up(s):
        acc_g[...] += jnp.dot(nrm[:, columns(pos - s, chunk)], wg[s], preferred_element_type=F32)
        acc_u[...] += jnp.dot(nrm[:, columns(pos + s, chunk)], wu[s], preferred_element_type=F32)

    acc_g[...] = jnp.zeros_like(acc_g)
    acc_u[...] = jnp.zeros_like(acc_u)

    def w_caught_up(s, carry):
        gate_up(s)
        return carry

    def w_step(s, carry):
        tick(w_copy, s)
        gate_up(s)
        return carry

    lax.fori_loop(0, 2 * early + 1, w_caught_up, 0)
    lax.fori_loop(2 * early + 1, n - 1, w_step, 0)
    tick(w_copy, n - 1, following=d_copy)
    gate_up(n - 1)

    width = acc_g.shape[1]
    joined[:, :width] = acc_g[...].astype(BF16)
    joined[:, width:] = acc_u[...].astype(BF16)
    edge = halo_lo.shape[0]
    up_copy = remote(
        joined.at[pl.ds(rows - edge, edge)], halo_lo, h_send.at[0], h_recv.at[0], sp=above
    )
    down_copy = remote(joined.at[pl.ds(0, edge)], halo_hi, h_send.at[1], h_recv.at[1], sp=below)
    up_copy.start()
    down_copy.start()

    def d_tick(s, carry):
        tick(d_copy, s)
        return carry

    lax.fori_loop(1, 2, d_tick, 0)
    up_copy.wait_recv()
    down_copy.wait_recv()
    has_low = jnp.where(sp > 0, F32(1.0), F32(0.0))
    has_high = jnp.where(sp < n - 1, F32(1.0), F32(0.0))

    def convolved(start, taps_ref):
        cut = slice(start, start + width)
        now = joined[:, cut].astype(F32)
        low = halo_lo[:, cut].astype(F32)[edge - 1:edge] * has_low
        high = halo_hi[:, cut].astype(F32)[0:1] * has_high
        line = lax.broadcasted_iota(jnp.int32, now.shape, 0)
        before = jnp.where(line == 0, low, pltpu.roll(now, 1, 0))
        after = jnp.where(line == rows - 1, high, pltpu.roll(now, rows - 1, 0))
        taps = taps_ref[...]
        return before * taps[0:1] + now * taps[1:2] + after * taps[2:3]

    gate = convolved(0, cg_ref)
    up = convolved(width, cu_ref)
    hidden[...] = (gate / (1.0 + jnp.exp(-gate)) * up).astype(BF16)

    dcols = wdr.shape[2]
    split = wdr.shape[1]
    acc_d[...] = jnp.zeros_like(acc_d)

    def down(s):
        acc_d[at(pos - s)] += jnp.dot(hidden[:, :split], wdr[s], preferred_element_type=F32)
        acc_d[at(pos + s)] += jnp.dot(hidden[:, split:], wdl[s], preferred_element_type=F32)

    def r2_copy(r, d):
        block = at(pos - r)
        to = lax.rem(tp + d, tp_n)
        return remote(
            part2.at[block, pl.ds(pl.multiple_of(to * own, own), own)], rs2_in.at[d - 1, block],
            r2_send.at[r, d - 1], r2_recv.at[r, d - 1], tp=to,
        )

    def give(r):
        block = at(pos - r)
        part2[block] = acc_d[block].astype(BF16)
        for d in range(1, tp_n):
            r2_copy(r, d).start()

    def d_caught_up(s, carry):
        down(s)
        return carry

    def d_step(s, carry):
        tick(d_copy, s)
        down(s)
        return carry

    def d_step_give(s, carry):
        tick(d_copy, s)
        down(s)
        give(s)
        give(n - s)
        return carry

    lax.fori_loop(0, 2, d_caught_up, 0)
    lax.fori_loop(2, half, d_step, 0)
    give(0)
    tick(d_copy, half)
    down(half)
    give(half)
    lax.fori_loop(half + 1, n - 1, d_step_give, 0)
    tick(d_copy, n - 1, following="end")
    down(n - 1)
    give(n - 1)
    give(1)

    def sent_r(s, carry):
        kv_r(s).wait_send()
        return carry

    def sent_l(s, carry):
        kv_l(s).wait_send()
        return carry

    def sent_w(s, carry):
        for p in range(PIECES):
            for direction in range(2):
                w_copy(s, p, direction).wait_send()
                d_copy(s, p, direction).wait_send()
        return carry

    lax.fori_loop(1, half + 1, sent_r, 0)
    lax.fori_loop(1, half, sent_l, 0)
    lax.fori_loop(1, n, sent_w, 0)
    up_copy.wait_send()
    down_copy.wait_send()
    for d in range(1, tp_n):
        rs_copy(d).wait_send()
        ag_copy(d).wait_send()

    def arrived(r, carry):
        for d in range(1, tp_n):
            r2_copy(r, d).wait_send()
            r2_copy(r, d).wait_recv()
        return carry

    lax.fori_loop(0, n, arrived, 0)
    for block in range(n):
        cut = slice(block * dcols, (block + 1) * dcols)
        summed = part2[block, mine].astype(F32)
        for d in range(1, tp_n):
            summed = summed + rs2_in[d - 1, block].astype(F32)
        out_ref[:, cut] = (mid[:, cut] + summed).astype(out_ref.dtype)


def on_device(n, tp_n, *args):
    if n % 2 or n < 8 or args[14].shape[0] % 128 or args[18].shape[1] % 128:
        return on_device_narrow(*args)
    (x_res, q_a, k_a, v_a, q_b, k_b, v_b, gain_qa, gain_ka, gain_qb, gain_kb, w_out_a, w_out_b,
     gain_mid, w_gate, w_up, conv_gate, conv_up, w_down) = args
    rows = q_a.shape[0]
    own, width = x_res.shape
    ff = w_gate.shape[1]
    heads_a, heads_b = q_a.shape[1] // DHA, q_b.shape[1] // DHB
    positions = lax.axis_index("sp") * rows + lax.iota(jnp.int32, rows)
    angle_a = rotary_angles(positions, DHA)
    angle_a = jnp.concatenate([angle_a, angle_a], axis=1)
    angle_b = rotary_angles(positions, DHB)
    cos_a, sin_a, cos_b, sin_b = jnp.cos(angle_a), jnp.sin(angle_a), jnp.cos(angle_b), jnp.sin(angle_b)
    vmem = pl.BlockSpec(memory_space=pltpu.VMEM)
    hbm = pl.BlockSpec(memory_space=pltpu.MemorySpace.HBM)
    edge = 16
    kv_width = 2 * k_a.shape[1] + 2 * k_b.shape[1]
    dma = pltpu.SemaphoreType.DMA
    scratch = [
        pltpu.VMEM((n, rows, kv_width), BF16),
        pltpu.VMEM((heads_a, rows, DHA), BF16),
        pltpu.VMEM((heads_b, rows, DHB), BF16),
        pltpu.VMEM((heads_a, rows, 1), F32),
        pltpu.VMEM((heads_a, rows, 1), F32),
        pltpu.VMEM((heads_a, rows, DHA), F32),
        pltpu.VMEM((heads_b, rows, 1), F32),
        pltpu.VMEM((heads_b, rows, 1), F32),
        pltpu.VMEM((heads_b, rows, DHB), F32),
        pltpu.VMEM(w_out_a.shape, BF16),
        pltpu.VMEM(w_out_b.shape, BF16),
        pltpu.VMEM((n,) + w_gate.shape, BF16),
        pltpu.VMEM((n,) + w_up.shape, BF16),
        pltpu.VMEM((n, ff // 2, w_down.shape[1]), BF16),
        pltpu.VMEM((n, ff // 2, w_down.shape[1]), BF16),
        pltpu.VMEM((rows, q_a.shape[1] + q_b.shape[1]), BF16),
        pltpu.VMEM((rows, width), BF16),
        pltpu.VMEM((tp_n - 1, own, width), BF16),
        pltpu.VMEM((own, width), F32),
        pltpu.VMEM((rows, width), BF16),
        pltpu.VMEM((rows, ff), F32),
        pltpu.VMEM((rows, ff), F32),
        pltpu.VMEM((rows, 2 * ff), BF16),
        pltpu.VMEM((edge, 2 * ff), BF16),
        pltpu.VMEM((edge, 2 * ff), BF16),
        pltpu.VMEM((rows, ff), BF16),
        pltpu.VMEM((n, rows, w_down.shape[1]), F32),
        pltpu.VMEM((n, rows, w_down.shape[1]), BF16),
        pltpu.VMEM((tp_n - 1, n, own, w_down.shape[1]), BF16),
        dma((6,)),
        dma((n,)), dma((n,)),
        dma((2, PIECES, n)), dma((2, PIECES, n)),
        dma((2, PIECES, n)), dma((2, PIECES, n)),
        dma((tp_n - 1,)), dma((tp_n - 1,)),
        dma((tp_n - 1,)), dma((tp_n - 1,)),
        dma((2,)), dma((2,)),
        dma((n, tp_n - 1)), dma((n, tp_n - 1)),
    ]
    return pl.pallas_call(
        functools.partial(kernel, n, tp_n),
        out_shape=jax.ShapeDtypeStruct(x_res.shape, BF16),
        in_specs=[vmem] * 15 + [hbm, hbm, vmem, hbm, hbm, vmem, vmem, hbm],
        out_specs=vmem,
        scratch_shapes=scratch,
        compiler_params=pltpu.CompilerParams(
            collective_id=0, has_side_effects=True, vmem_limit_bytes=60 * 1024 * 1024
        ),
        name="layer",
    )(
        x_res, q_a, k_a, v_a, q_b, k_b, v_b,
        gain_qa[None], gain_ka[None], gain_qb[None], gain_kb[None],
        cos_a, sin_a, cos_b, sin_b,
        w_out_a, w_out_b, gain_mid[None], w_gate, w_up, conv_gate, conv_up, w_down,
    )


def extended(block, sides, width):
    for axis, dim in sides:
        count = lax.axis_size(axis)
        forward = [(i, i + 1) for i in range(count - 1)]
        backward = [(target, source) for source, target in forward]
        low = lax.ppermute(
            lax.slice_in_dim(block, block.shape[dim] - width, None, axis=dim), axis, forward
        )
        high = lax.ppermute(lax.slice_in_dim(block, 0, width, axis=dim), axis, backward)
        block = jnp.concatenate([low, block, high], axis=dim)
    return block


def rotate_half(values):
    first, second = jnp.split(values, 2, axis=-1)
    return jnp.concatenate([-second, first], axis=-1)


def prepare(raw, gain, head_size, positions):
    count = raw.shape[0]
    heads = raw.shape[1] // head_size
    values = raw.astype(jnp.float32).reshape(count, heads, head_size)
    values = values * lax.rsqrt(jnp.mean(values * values, axis=-1, keepdims=True) + norm_eps)
    values = values * gain
    angles = rotary_angles(positions, head_size)
    cosine, sine = jnp.cos(angles), jnp.sin(angles)
    row_part, col_part = jnp.split(values, 2, axis=-1)
    turned = jnp.concatenate([rotate_half(row_part), rotate_half(col_part)], axis=-1)
    values = values * cosine[:, None, :] + turned * sine[:, None, :]
    return values.astype(jnp.bfloat16)


def start_state(queries):
    count, kv_heads, groups, head_size = queries.shape
    lowest = jnp.full((kv_heads, groups, count), -1e30, jnp.float32)
    totals = jnp.zeros((kv_heads, groups, count), jnp.float32)
    summed = jnp.zeros((kv_heads, groups, count, head_size), jnp.float32)
    return (lowest, totals, summed)


def attend(state, queries, key_piece, value_piece):
    head_size = queries.shape[3]
    kv_heads = queries.shape[1]
    length = key_piece.shape[0]
    keys = key_piece.reshape(length, kv_heads, head_size)
    values = value_piece.reshape(length, kv_heads, head_size)
    span = length
    while span > 1024 and span % 2 == 0:
        span = span // 2
    scale = jnp.float32(head_size ** (-0.5))

    def one_span(index, carry):
        running, totals, summed = carry
        key_rows = lax.dynamic_slice_in_dim(keys, index * span, span, 0)
        value_rows = lax.dynamic_slice_in_dim(values, index * span, span, 0)
        scores = (
            jnp.einsum("qkgd,skd->kgqs", queries, key_rows, preferred_element_type=jnp.float32)
            * scale
        )
        highest = jnp.maximum(running, jnp.max(scores, axis=-1))
        factor = jnp.exp(running - highest)
        expd = jnp.exp(scores - highest[..., None])
        totals = totals * factor + jnp.sum(expd, axis=-1)
        summed = summed * factor[..., None] + jnp.einsum(
            "kgqs,skd->kgqd",
            expd.astype(jnp.bfloat16),
            value_rows,
            preferred_element_type=jnp.float32,
        )
        return (highest, totals, summed)

    return lax.fori_loop(0, length // span, one_span, state)


def finish(state):
    running, totals, summed = state
    kv_heads, groups, count, head_size = summed.shape
    result = summed / totals[..., None]
    return (
        jnp.transpose(result, (2, 0, 1, 3))
        .reshape(count, kv_heads * groups * head_size)
        .astype(jnp.bfloat16)
    )


def on_device_narrow(
    x_res,
    q_a,
    k_a,
    v_a,
    q_b,
    k_b,
    v_b,
    gain_qa,
    gain_ka,
    gain_qb,
    gain_kb,
    w_out_a,
    w_out_b,
    gain_mid,
    w_gate,
    w_up,
    conv_gate,
    conv_up,
    w_down,
):
    tok_rows = q_a.shape[0]
    whole_gate, whole_up, whole_down = (
        lax.all_gather(w_gate, "sp", axis=0, tiled=True),
        lax.all_gather(w_up, "sp", axis=0, tiled=True),
        lax.all_gather(w_down, "sp", axis=1, tiled=True),
    )
    positions = lax.axis_index("sp") * tok_rows + lax.iota(jnp.int32, tok_rows)
    kv_a = k_a.shape[1] // DHA
    kv_b = k_b.shape[1] // DHB
    query_a = prepare(q_a, gain_qa, DHA, positions)
    query_a = query_a.reshape(tok_rows, kv_a, query_a.shape[1] // kv_a, DHA)
    query_b = prepare(q_b, gain_qb, DHB, positions)
    query_b = query_b.reshape(tok_rows, kv_b, query_b.shape[1] // kv_b, DHB)
    keys_a = prepare(k_a, gain_ka, DHA, positions).reshape(tok_rows, kv_a * DHA)
    keys_b = prepare(k_b, gain_kb, DHB, positions).reshape(tok_rows, kv_b * DHB)
    state_a = attend(
        start_state(query_a),
        query_a,
        lax.all_gather(keys_a, "sp", axis=0, tiled=True),
        lax.all_gather(v_a, "sp", axis=0, tiled=True),
    )
    state_b = attend(
        start_state(query_b),
        query_b,
        lax.all_gather(keys_b, "sp", axis=0, tiled=True),
        lax.all_gather(v_b, "sp", axis=0, tiled=True),
    )
    attn_a = finish(state_a)
    attn_b = finish(state_b)
    projected = lax.psum_scatter(
        (
            jnp.dot(attn_a, w_out_a, preferred_element_type=jnp.float32)
            + jnp.dot(attn_b, w_out_b, preferred_element_type=jnp.float32)
        ).astype(jnp.bfloat16),
        "tp",
        scatter_dimension=0,
        tiled=True,
    ).astype(jnp.float32)
    middle = x_res.astype(jnp.float32) + projected
    normed = middle * lax.rsqrt(jnp.mean(middle * middle, axis=-1, keepdims=True) + norm_eps)
    normed = (normed * gain_mid).astype(jnp.bfloat16)
    gathered = lax.all_gather(normed, "tp", axis=0, tiled=True)
    gate_pre = jnp.dot(gathered, whole_gate, preferred_element_type=jnp.float32)
    up_pre = jnp.dot(gathered, whole_up, preferred_element_type=jnp.float32)
    width = gate_pre.shape[1]
    joined = jnp.concatenate([gate_pre, up_pre], axis=1).astype(jnp.bfloat16)
    padded = extended(joined, (("sp", 0),), 1)
    taps = jnp.concatenate([conv_gate, conv_up], axis=1)
    mixed = padded[:-2] * taps[0] + padded[1:-1] * taps[1] + padded[2:] * taps[2]
    hidden = (jax.nn.silu(mixed[:, :width]) * mixed[:, width:]).astype(jnp.bfloat16)
    terms = jnp.dot(hidden, whole_down, preferred_element_type=jnp.float32)
    summed = lax.psum_scatter(
        terms.astype(jnp.bfloat16), "tp", scatter_dimension=0, tiled=True
    ).astype(jnp.float32)
    return (middle + summed).astype(jnp.bfloat16)


def solution(mesh):
    in_specs = (
        P(("sp", "tp"), None),
        P("sp", "tp"),
        P("sp", "tp"),
        P("sp", "tp"),
        P("sp", "tp"),
        P("sp", "tp"),
        P("sp", "tp"),
        P(),
        P(),
        P(),
        P(),
        P("tp", None),
        P("tp", None),
        P(),
        P("sp", "tp"),
        P("sp", "tp"),
        P(None, "tp"),
        P(None, "tp"),
        P("tp", "sp"),
    )
    out_specs = P(("sp", "tp"), None)
    body = functools.partial(on_device, mesh.shape["sp"], mesh.shape["tp"])
    return jax.shard_map(
        body, mesh=mesh, in_specs=in_specs, out_specs=out_specs, check_vma=False
    )
```

```python
import functools

import jax
import jax.numpy as jnp
from jax import lax
from jax.experimental import pallas as pl
from jax.experimental.pallas import tpu as pltpu
from jax.sharding import PartitionSpec as P

DHA = 64
DHB = 128

norm_eps = 1e-06
rope_theta = 10000.0
F32 = jnp.float32
BF16 = jnp.bfloat16
MESH = pl.DeviceIdType.MESH
PIECES = 4


def rotary_angles(positions, head_size):
    half = head_size // 2
    inverse = jnp.power(jnp.float32(rope_theta), -jnp.arange(0, half, 2, dtype=jnp.float32) / half)
    grid_row = (positions // 64).astype(jnp.float32)[:, None] * inverse[None, :]
    grid_col = (positions % 64).astype(jnp.float32)[:, None] * inverse[None, :]
    return jnp.concatenate([grid_row, grid_row, grid_col, grid_col], axis=-1)


def lane_frequencies(head_size, width):
    half = head_size // 2
    inverse = jnp.power(jnp.float32(rope_theta), -jnp.arange(0, half, 2, dtype=jnp.float32) / half)
    return jnp.tile(inverse, width // inverse.shape[0])[None]


def block_mean(width, head):
    i = lax.broadcasted_iota(jnp.int32, (width, width), 0)
    j = lax.broadcasted_iota(jnp.int32, (width, width), 1)
    return jnp.where(lax.div(i, head) == lax.div(j, head), F32(1.0 / head), F32(0.0))


def block_turn(width, head):
    quarter = head // 4
    i = lax.broadcasted_iota(jnp.int32, (width, width), 0)
    j = lax.broadcasted_iota(jnp.int32, (width, width), 1)
    first = lax.rem(j, 2 * quarter) < quarter
    return jnp.where(
        first & (i == j + quarter),
        F32(-1.0),
        jnp.where(jnp.logical_not(first) & (i == j - quarter), F32(1.0), F32(0.0)),
    )


def exact_dot(a, b):
    return jnp.dot(a, b, precision=lax.Precision.HIGHEST, preferred_element_type=F32)


def prepared(raw, gain, angle_cos, angle_sin, head):
    width = raw.shape[1]
    values = raw.astype(F32)
    values = values * lax.rsqrt(exact_dot(values * values, block_mean(width, head)) + norm_eps)
    values = values * gain
    turned = exact_dot(values, block_turn(width, head))
    return (values * angle_cos + turned * angle_sin).astype(BF16)


def kernel(
    n, tp_n,
    x_ref, qa_ref, ka_hbm, va_hbm, qb_ref, kb_ref, vb_ref,
    gqa_ref, gka_ref, gqb_ref, gkb_ref,
    fra_ref, frb_ref,
    woa_hbm, wob_hbm, gmid_ref, wg_hbm, wu_hbm, cg_ref, cu_ref, wd_hbm,
    out_ref,
    ka_ref, va_ref, kv, qas, qbs, m_a, l_a, acc_a, m_b, l_b, acc_b,
    woa, wob, wg, wu, wdr, wdl,
    attn, part, rs_in, mid, nrm, acc_g, acc_u, joined, halo_lo, halo_hi, hidden, acc_d, part2, rs2_in,
    loc_sem, kv_send, kv_recv, w_send, w_recv, d_send, d_recv,
    rs_send, rs_recv, ag_send, ag_recv, h_send, h_recv, r2_send, r2_recv,
):
    sp = lax.axis_index("sp")
    tp = lax.axis_index("tp")
    rows = qa_ref.shape[0]
    own = x_ref.shape[0]
    half = n // 2

    odd = lax.rem(sp, 2)
    pos = (1 - odd) * lax.div(sp, 2) + odd * (n - 1 - lax.div(sp, 2))

    def at(p):
        p = lax.rem(p + 2 * n, n)
        back = lax.div(p, half)
        return (1 - back) * 2 * p + back * (2 * (n - 1 - p) + 1)

    right, left = at(pos + 1), at(pos - 1)
    above, below = lax.rem(sp + 1, n), lax.rem(sp + n - 1, n)

    barrier = pltpu.get_barrier_semaphore()
    for other in (right, left, above, below):
        pl.semaphore_signal(barrier, inc=1, device_id={"sp": other}, device_id_type=MESH)
    for d in range(1, tp_n):
        pl.semaphore_signal(
            barrier, inc=1, device_id={"tp": lax.rem(tp + d, tp_n)}, device_id_type=MESH
        )

    locals_ = [
        pltpu.make_async_copy(woa_hbm, woa, loc_sem.at[0]),
        pltpu.make_async_copy(wob_hbm, wob, loc_sem.at[1]),
        pltpu.make_async_copy(wg_hbm, wg.at[0], loc_sem.at[2]),
        pltpu.make_async_copy(wu_hbm, wu.at[0], loc_sem.at[3]),
        pltpu.make_async_copy(wd_hbm.at[pl.ds(0, wdr.shape[1])], wdr.at[0], loc_sem.at[4]),
        pltpu.make_async_copy(
            wd_hbm.at[pl.ds(wdr.shape[1], wdr.shape[1])], wdl.at[0], loc_sem.at[5]
        ),
    ]
    small = [
        pltpu.make_async_copy(ka_hbm, ka_ref, loc_sem.at[6]),
        pltpu.make_async_copy(va_hbm, va_ref, loc_sem.at[7]),
    ]
    for copy in locals_[2:4] + small + locals_[4:] + locals_[:2]:
        copy.start()

    def remote(src, dst, send, recv, **where):
        return pltpu.make_async_remote_copy(
            src_ref=src, dst_ref=dst, send_sem=send, recv_sem=recv,
            device_id=where, device_id_type=MESH,
        )

    def kv_r(s):
        return remote(kv.at[s - 1], kv.at[s], kv_send.at[s], kv_recv.at[s], sp=right)

    def kv_l(s):
        source = lax.rem(n - s + 1, n)
        return remote(kv.at[source], kv.at[n - s], kv_send.at[n - s], kv_recv.at[n - s], sp=left)

    wrows = wg.shape[1] // PIECES
    drows = wdr.shape[1] // PIECES

    def w_copy(s, p, direction):
        buf, to = (wg, right) if direction == 0 else (wu, left)
        cut = pl.ds(p * wrows, wrows)
        return remote(
            buf.at[s - 1, cut], buf.at[s, cut],
            w_send.at[direction, p, s], w_recv.at[direction, p, s], sp=to,
        )

    def d_copy(s, p, direction):
        buf, to = (wdr, right) if direction == 0 else (wdl, left)
        cut = pl.ds(p * drows, drows)
        return remote(
            buf.at[s - 1, cut], buf.at[s, cut],
            d_send.at[direction, p, s], d_recv.at[direction, p, s], sp=to,
        )

    def tick(copy, s, following=None):
        for p in range(PIECES):
            for direction in range(2):
                copy(s, p, direction).wait_recv()
                if following is None:
                    copy(s + 1, p, direction).start()
                elif following != "end":
                    following(1, p, direction).wait_recv()
                    following(2, p, direction).start()

    def begin(copy, s, low, high):
        for p in range(low, high):
            for direction in range(2):
                copy(s, p, direction).start()

    def pass_on(copy, s, low, high):
        for p in range(low, high):
            for direction in range(2):
                copy(s, p, direction).wait_recv()
                copy(s + 1, p, direction).start()

    pl.semaphore_wait(barrier, 4 + tp_n - 1)
    for copy in locals_[2:4]:
        copy.wait()
    begin(w_copy, 1, 0, PIECES // 2)

    def tables(freq_ref, head):
        shape = (rows, freq_ref.shape[1])
        token = lax.broadcasted_iota(jnp.int32, shape, 0) + sp * rows
        lane = lax.broadcasted_iota(jnp.int32, shape, 1)
        grid = jnp.where(lax.rem(lane, head) < head // 2, lax.div(token, 64), lax.rem(token, 64))
        angles = grid.astype(F32) * freq_ref[...]
        return jnp.cos(angles), jnp.sin(angles)

    ca, sa = tables(fra_ref, DHA)
    cb, sb = tables(frb_ref, DHB)
    for copy in small:
        copy.wait()
    wka, wkb = ka_ref.shape[1], kb_ref.shape[1]

    def wide(table, width):
        if width <= table.shape[1]:
            return table[:, :width]
        return jnp.concatenate([table] * (width // table.shape[1]), axis=1)

    def gains(ref, width):
        g = ref[...]
        count = width // g.shape[1]
        return g if count == 1 else jnp.concatenate([g] * count, axis=1)

    keys_a = prepared(ka_ref[...], gains(gka_ref, wka), wide(ca, wka), wide(sa, wka), DHA)
    keys_b = prepared(kb_ref[...], gains(gkb_ref, wkb), wide(cb, wkb), wide(sb, wkb), DHB)
    kv[0, :, :wkb] = keys_b
    kv[0, :, wkb:2 * wkb] = vb_ref[...]
    kv[0, :, 2 * wkb:] = jnp.concatenate([keys_a, va_ref[...]], axis=1)

    kv_r(1).start()
    kv_l(1).start()

    heads_a = qa_ref.shape[1] // DHA
    heads_b = qb_ref.shape[1] // DHB
    qa = prepared(
        qa_ref[...], gains(gqa_ref, heads_a * DHA), wide(ca, heads_a * DHA),
        wide(sa, heads_a * DHA), DHA,
    )
    qb = prepared(
        qb_ref[...], gains(gqb_ref, heads_b * DHB), wide(cb, heads_b * DHB),
        wide(sb, heads_b * DHB), DHB,
    )
    for h in range(heads_a):
        qas[h] = qa[:, h * DHA:(h + 1) * DHA]
    for h in range(heads_b):
        qbs[h] = qb[:, h * DHB:(h + 1) * DHB]
    for ref, low in ((m_a, -1e30), (m_b, -1e30), (l_a, 0.0), (l_b, 0.0), (acc_a, 0.0), (acc_b, 0.0)):
        ref[...] = jnp.full(ref.shape, low, F32)

    def attend_one(queries, key_rows, value_rows, m, l, acc, h):
        scale = F32(queries.shape[2] ** (-0.5))
        scores = lax.dot_general(
            queries[h], key_rows, (((1,), (1,)), ((), ())), preferred_element_type=F32
        ) * scale
        before = m[h]
        highest = jnp.maximum(before, jnp.max(scores, axis=-1, keepdims=True))
        factor = jnp.exp(before - highest)
        expd = jnp.exp(scores - highest)
        l[h] = l[h] * factor + jnp.sum(expd, axis=-1, keepdims=True)
        acc[h] = acc[h] * factor + jnp.dot(
            expd.astype(BF16), value_rows, preferred_element_type=F32
        )
        m[h] = highest

    def attend(slot):
        for h in range(heads_b):
            attend_one(qbs, kv[slot, :, :wkb], kv[slot, :, wkb:2 * wkb], m_b, l_b, acc_b, h)
        pair = kv[slot, :, 2 * wkb:]
        for h in range(heads_a):
            attend_one(qas, pair[:, :wka], pair[:, wka:], m_a, l_a, acc_a, h)

    attend(0)

    def kv_step(s, carry):
        kv_r(s).wait_recv()
        kv_r(s + 1).start()
        kv_l(s).wait_recv()

        @pl.when(s < half - 1)
        def _():
            kv_l(s + 1).start()

        @pl.when(s == 1)
        def _():
            begin(w_copy, 1, PIECES // 2, PIECES)

        @pl.when(s == 2)
        def _():
            begin(d_copy, 1, 0, PIECES)

        @pl.when(s == 3)
        def _():
            pass_on(w_copy, 1, 0, PIECES // 2)

        def one(i, inner):
            attend((1 - i) * s + i * (n - s))
            return inner

        lax.fori_loop(0, 2, one, 0)
        return carry

    for copy in locals_[:2] + locals_[4:]:
        copy.wait()
    lax.fori_loop(1, half, kv_step, 0)
    kv_r(half).wait_recv()
    pass_on(w_copy, 1, PIECES // 2, PIECES)
    attend(half)

    for h in range(heads_a):
        attn[:, h * DHA:(h + 1) * DHA] = (acc_a[h] / l_a[h]).astype(BF16)
    width_a = heads_a * DHA
    for h in range(heads_b):
        attn[:, width_a + h * DHB:width_a + (h + 1) * DHB] = (acc_b[h] / l_b[h]).astype(BF16)

    def rs_copy(d):
        to = lax.rem(tp + d, tp_n)
        return remote(
            part.at[pl.ds(pl.multiple_of(to * own, own), own)], rs_in.at[d - 1],
            rs_send.at[d - 1], rs_recv.at[d - 1], tp=to,
        )

    for i in range(tp_n):
        d = tp_n - 1 - i
        at_rows = pl.ds(pl.multiple_of(lax.rem(tp + d, tp_n) * own, own), own)
        block = attn[at_rows, :]
        part[at_rows, :] = (
            jnp.dot(block[:, :width_a], woa[...], preferred_element_type=F32)
            + jnp.dot(block[:, width_a:], wob[...], preferred_element_type=F32)
        ).astype(BF16)
        if d > 0:
            rs_copy(d).start()

    def w_tick(s, carry):
        tick(w_copy, s)
        return carry

    lax.fori_loop(2, 4, w_tick, 0)

    mine = pl.ds(pl.multiple_of(tp * own, own), own)
    total = part[mine, :].astype(F32)
    for d in range(1, tp_n):
        rs_copy(d).wait_recv()
        total = total + rs_in[d - 1].astype(F32)
    middle = x_ref[...].astype(F32) + total
    mid[...] = middle
    normed = middle * lax.rsqrt(jnp.mean(middle * middle, axis=-1, keepdims=True) + norm_eps)
    nrm[mine, :] = (normed * gmid_ref[...]).astype(BF16)

    def ag_copy(d):
        return remote(
            nrm.at[mine], nrm.at[mine], ag_send.at[d - 1], ag_recv.at[d - 1],
            tp=lax.rem(tp + d, tp_n),
        )

    for d in range(1, tp_n):
        ag_copy(d).start()
    lax.fori_loop(4, 6, w_tick, 0)
    for d in range(1, tp_n):
        ag_copy(d).wait_recv()

    chunk = wg.shape[1]

    def columns(p, width):
        return pl.ds(pl.multiple_of(at(p) * width, width), width)

    def gate_up(s):
        acc_g[...] += jnp.dot(nrm[:, columns(pos - s, chunk)], wg[s], preferred_element_type=F32)
        acc_u[...] += jnp.dot(nrm[:, columns(pos + s, chunk)], wu[s], preferred_element_type=F32)

    acc_g[...] = jnp.zeros_like(acc_g)
    acc_u[...] = jnp.zeros_like(acc_u)

    def w_caught_up(s, carry):
        gate_up(s)
        return carry

    def w_step(s, carry):
        tick(w_copy, s)
        gate_up(s)
        return carry

    lax.fori_loop(0, 4, w_caught_up, 0)
    lax.fori_loop(6, n - 1, w_step, 0)
    lax.fori_loop(4, 6, w_caught_up, 0)
    tick(w_copy, n - 1, following=d_copy)
    gate_up(n - 1)

    width = acc_g.shape[1]
    joined[:, :width] = acc_g[...].astype(BF16)
    joined[:, width:] = acc_u[...].astype(BF16)
    edge = halo_lo.shape[0]
    up_copy = remote(
        joined.at[pl.ds(rows - edge, edge)], halo_lo, h_send.at[0], h_recv.at[0], sp=above
    )
    down_copy = remote(joined.at[pl.ds(0, edge)], halo_hi, h_send.at[1], h_recv.at[1], sp=below)
    up_copy.start()
    down_copy.start()

    tick(d_copy, 2)
    up_copy.wait_recv()
    down_copy.wait_recv()
    has_low = jnp.where(sp > 0, F32(1.0), F32(0.0))
    has_high = jnp.where(sp < n - 1, F32(1.0), F32(0.0))

    def convolved(start, taps_ref):
        cut = slice(start, start + width)
        now = joined[:, cut].astype(F32)
        low = halo_lo[:, cut].astype(F32)[edge - 1:edge] * has_low
        high = halo_hi[:, cut].astype(F32)[0:1] * has_high
        line = lax.broadcasted_iota(jnp.int32, now.shape, 0)
        before = jnp.where(line == 0, low, pltpu.roll(now, 1, 0))
        after = jnp.where(line == rows - 1, high, pltpu.roll(now, rows - 1, 0))
        taps = taps_ref[...]
        return before * taps[0:1] + now * taps[1:2] + after * taps[2:3]

    gate = convolved(0, cg_ref)
    acc_g[...] = gate / (1.0 + jnp.exp(-gate))
    tick(d_copy, 3)
    hidden[...] = (acc_g[...] * convolved(width, cu_ref)).astype(BF16)

    dcols = wdr.shape[2]
    split = wdr.shape[1]
    acc_d[...] = jnp.zeros_like(acc_d)

    def down(s):
        acc_d[at(pos - s)] += jnp.dot(hidden[:, :split], wdr[s], preferred_element_type=F32)
        acc_d[at(pos + s)] += jnp.dot(hidden[:, split:], wdl[s], preferred_element_type=F32)

    def r2_copy(r, d):
        block = at(pos - r)
        to = lax.rem(tp + d, tp_n)
        return remote(
            part2.at[block, pl.ds(pl.multiple_of(to * own, own), own)], rs2_in.at[d - 1, block],
            r2_send.at[r, d - 1], r2_recv.at[r, d - 1], tp=to,
        )

    def give(r):
        block = at(pos - r)
        part2[block] = acc_d[block].astype(BF16)
        for d in range(1, tp_n):
            r2_copy(r, d).start()

    def d_caught_up(s, carry):
        down(s)
        return carry

    def d_step(s, carry):
        tick(d_copy, s)
        down(s)
        return carry

    def d_step_give(s, carry):
        tick(d_copy, s)
        down(s)
        give(s)
        give(n - s)
        return carry

    lax.fori_loop(0, 4, d_caught_up, 0)
    lax.fori_loop(4, half, d_step, 0)
    give(0)
    tick(d_copy, half)
    down(half)
    give(half)
    lax.fori_loop(half + 1, n - 1, d_step_give, 0)
    tick(d_copy, n - 1, following="end")
    down(n - 1)
    give(n - 1)
    give(1)

    def sent_r(s, carry):
        kv_r(s).wait_send()
        return carry

    def sent_l(s, carry):
        kv_l(s).wait_send()
        return carry

    def sent_w(s, carry):
        for p in range(PIECES):
            for direction in range(2):
                w_copy(s, p, direction).wait_send()
                d_copy(s, p, direction).wait_send()
        return carry

    lax.fori_loop(1, half + 1, sent_r, 0)
    lax.fori_loop(1, half, sent_l, 0)
    lax.fori_loop(1, n, sent_w, 0)
    up_copy.wait_send()
    down_copy.wait_send()
    for d in range(1, tp_n):
        rs_copy(d).wait_send()
        ag_copy(d).wait_send()

    def arrived(r, carry):
        for d in range(1, tp_n):
            r2_copy(r, d).wait_send()
            r2_copy(r, d).wait_recv()
        return carry

    lax.fori_loop(0, n, arrived, 0)
    for block in range(n):
        cut = slice(block * dcols, (block + 1) * dcols)
        summed = part2[block, mine].astype(F32)
        for d in range(1, tp_n):
            summed = summed + rs2_in[d - 1, block].astype(F32)
        out_ref[:, cut] = (mid[:, cut] + summed).astype(out_ref.dtype)


def on_device(n, tp_n, *args):
    if n % 2 or n < 8 or args[14].shape[0] % 128 or args[18].shape[1] % 128:
        return on_device_narrow(*args)
    (x_res, q_a, k_a, v_a, q_b, k_b, v_b, gain_qa, gain_ka, gain_qb, gain_kb, w_out_a, w_out_b,
     gain_mid, w_gate, w_up, conv_gate, conv_up, w_down) = args
    rows = q_a.shape[0]
    own, width = x_res.shape
    ff = w_gate.shape[1]
    heads_a, heads_b = q_a.shape[1] // DHA, q_b.shape[1] // DHB
    freq_a, freq_b = lane_frequencies(DHA, 2 * DHA), lane_frequencies(DHB, DHB)
    vmem = pl.BlockSpec(memory_space=pltpu.VMEM)
    hbm = pl.BlockSpec(memory_space=pltpu.MemorySpace.HBM)
    edge = 16
    kv_width = 2 * k_a.shape[1] + 2 * k_b.shape[1]
    dma = pltpu.SemaphoreType.DMA
    scratch = [
        pltpu.VMEM(k_a.shape, BF16),
        pltpu.VMEM(v_a.shape, BF16),
        pltpu.VMEM((n, rows, kv_width), BF16),
        pltpu.VMEM((heads_a, rows, DHA), BF16),
        pltpu.VMEM((heads_b, rows, DHB), BF16),
        pltpu.VMEM((heads_a, rows, 1), F32),
        pltpu.VMEM((heads_a, rows, 1), F32),
        pltpu.VMEM((heads_a, rows, DHA), F32),
        pltpu.VMEM((heads_b, rows, 1), F32),
        pltpu.VMEM((heads_b, rows, 1), F32),
        pltpu.VMEM((heads_b, rows, DHB), F32),
        pltpu.VMEM(w_out_a.shape, BF16),
        pltpu.VMEM(w_out_b.shape, BF16),
        pltpu.VMEM((n,) + w_gate.shape, BF16),
        pltpu.VMEM((n,) + w_up.shape, BF16),
        pltpu.VMEM((n, ff // 2, w_down.shape[1]), BF16),
        pltpu.VMEM((n, ff // 2, w_down.shape[1]), BF16),
        pltpu.VMEM((rows, q_a.shape[1] + q_b.shape[1]), BF16),
        pltpu.VMEM((rows, width), BF16),
        pltpu.VMEM((tp_n - 1, own, width), BF16),
        pltpu.VMEM((own, width), F32),
        pltpu.VMEM((rows, width), BF16),
        pltpu.VMEM((rows, ff), F32),
        pltpu.VMEM((rows, ff), F32),
        pltpu.VMEM((rows, 2 * ff), BF16),
        pltpu.VMEM((edge, 2 * ff), BF16),
        pltpu.VMEM((edge, 2 * ff), BF16),
        pltpu.VMEM((rows, ff), BF16),
        pltpu.VMEM((n, rows, w_down.shape[1]), F32),
        pltpu.VMEM((n, rows, w_down.shape[1]), BF16),
        pltpu.VMEM((tp_n - 1, n, own, w_down.shape[1]), BF16),
        dma((8,)),
        dma((n,)), dma((n,)),
        dma((2, PIECES, n)), dma((2, PIECES, n)),
        dma((2, PIECES, n)), dma((2, PIECES, n)),
        dma((tp_n - 1,)), dma((tp_n - 1,)),
        dma((tp_n - 1,)), dma((tp_n - 1,)),
        dma((2,)), dma((2,)),
        dma((n, tp_n - 1)), dma((n, tp_n - 1)),
    ]
    return pl.pallas_call(
        functools.partial(kernel, n, tp_n),
        out_shape=jax.ShapeDtypeStruct(x_res.shape, BF16),
        in_specs=[vmem] * 2 + [hbm] * 2 + [vmem] * 9 + [hbm, hbm, vmem, hbm, hbm, vmem, vmem, hbm],
        out_specs=vmem,
        scratch_shapes=scratch,
        compiler_params=pltpu.CompilerParams(
            collective_id=0, has_side_effects=True, vmem_limit_bytes=60 * 1024 * 1024
        ),
        name="layer",
    )(
        x_res, q_a, k_a, v_a, q_b, k_b, v_b,
        gain_qa[None], gain_ka[None], gain_qb[None], gain_kb[None],
        freq_a, freq_b,
        w_out_a, w_out_b, gain_mid[None], w_gate, w_up, conv_gate, conv_up, w_down,
    )


def extended(block, sides, width):
    for axis, dim in sides:
        count = lax.axis_size(axis)
        forward = [(i, i + 1) for i in range(count - 1)]
        backward = [(target, source) for source, target in forward]
        low = lax.ppermute(
            lax.slice_in_dim(block, block.shape[dim] - width, None, axis=dim), axis, forward
        )
        high = lax.ppermute(lax.slice_in_dim(block, 0, width, axis=dim), axis, backward)
        block = jnp.concatenate([low, block, high], axis=dim)
    return block


def rotate_half(values):
    first, second = jnp.split(values, 2, axis=-1)
    return jnp.concatenate([-second, first], axis=-1)


def prepare(raw, gain, head_size, positions):
    count = raw.shape[0]
    heads = raw.shape[1] // head_size
    values = raw.astype(jnp.float32).reshape(count, heads, head_size)
    values = values * lax.rsqrt(jnp.mean(values * values, axis=-1, keepdims=True) + norm_eps)
    values = values * gain
    angles = rotary_angles(positions, head_size)
    cosine, sine = jnp.cos(angles), jnp.sin(angles)
    row_part, col_part = jnp.split(values, 2, axis=-1)
    turned = jnp.concatenate([rotate_half(row_part), rotate_half(col_part)], axis=-1)
    values = values * cosine[:, None, :] + turned * sine[:, None, :]
    return values.astype(jnp.bfloat16)


def start_state(queries):
    count, kv_heads, groups, head_size = queries.shape
    lowest = jnp.full((kv_heads, groups, count), -1e30, jnp.float32)
    totals = jnp.zeros((kv_heads, groups, count), jnp.float32)
    summed = jnp.zeros((kv_heads, groups, count, head_size), jnp.float32)
    return (lowest, totals, summed)


def attend(state, queries, key_piece, value_piece):
    head_size = queries.shape[3]
    kv_heads = queries.shape[1]
    length = key_piece.shape[0]
    keys = key_piece.reshape(length, kv_heads, head_size)
    values = value_piece.reshape(length, kv_heads, head_size)
    span = length
    while span > 1024 and span % 2 == 0:
        span = span // 2
    scale = jnp.float32(head_size ** (-0.5))

    def one_span(index, carry):
        running, totals, summed = carry
        key_rows = lax.dynamic_slice_in_dim(keys, index * span, span, 0)
        value_rows = lax.dynamic_slice_in_dim(values, index * span, span, 0)
        scores = (
            jnp.einsum("qkgd,skd->kgqs", queries, key_rows, preferred_element_type=jnp.float32)
            * scale
        )
        highest = jnp.maximum(running, jnp.max(scores, axis=-1))
        factor = jnp.exp(running - highest)
        expd = jnp.exp(scores - highest[..., None])
        totals = totals * factor + jnp.sum(expd, axis=-1)
        summed = summed * factor[..., None] + jnp.einsum(
            "kgqs,skd->kgqd",
            expd.astype(jnp.bfloat16),
            value_rows,
            preferred_element_type=jnp.float32,
        )
        return (highest, totals, summed)

    return lax.fori_loop(0, length // span, one_span, state)


def finish(state):
    running, totals, summed = state
    kv_heads, groups, count, head_size = summed.shape
    result = summed / totals[..., None]
    return (
        jnp.transpose(result, (2, 0, 1, 3))
        .reshape(count, kv_heads * groups * head_size)
        .astype(jnp.bfloat16)
    )


def on_device_narrow(
    x_res,
    q_a,
    k_a,
    v_a,
    q_b,
    k_b,
    v_b,
    gain_qa,
    gain_ka,
    gain_qb,
    gain_kb,
    w_out_a,
    w_out_b,
    gain_mid,
    w_gate,
    w_up,
    conv_gate,
    conv_up,
    w_down,
):
    tok_rows = q_a.shape[0]
    whole_gate, whole_up, whole_down = (
        lax.all_gather(w_gate, "sp", axis=0, tiled=True),
        lax.all_gather(w_up, "sp", axis=0, tiled=True),
        lax.all_gather(w_down, "sp", axis=1, tiled=True),
    )
    positions = lax.axis_index("sp") * tok_rows + lax.iota(jnp.int32, tok_rows)
    kv_a = k_a.shape[1] // DHA
    kv_b = k_b.shape[1] // DHB
    query_a = prepare(q_a, gain_qa, DHA, positions)
    query_a = query_a.reshape(tok_rows, kv_a, query_a.shape[1] // kv_a, DHA)
    query_b = prepare(q_b, gain_qb, DHB, positions)
    query_b = query_b.reshape(tok_rows, kv_b, query_b.shape[1] // kv_b, DHB)
    keys_a = prepare(k_a, gain_ka, DHA, positions).reshape(tok_rows, kv_a * DHA)
    keys_b = prepare(k_b, gain_kb, DHB, positions).reshape(tok_rows, kv_b * DHB)
    state_a = attend(
        start_state(query_a),
        query_a,
        lax.all_gather(keys_a, "sp", axis=0, tiled=True),
        lax.all_gather(v_a, "sp", axis=0, tiled=True),
    )
    state_b = attend(
        start_state(query_b),
        query_b,
        lax.all_gather(keys_b, "sp", axis=0, tiled=True),
        lax.all_gather(v_b, "sp", axis=0, tiled=True),
    )
    attn_a = finish(state_a)
    attn_b = finish(state_b)
    projected = lax.psum_scatter(
        (
            jnp.dot(attn_a, w_out_a, preferred_element_type=jnp.float32)
            + jnp.dot(attn_b, w_out_b, preferred_element_type=jnp.float32)
        ).astype(jnp.bfloat16),
        "tp",
        scatter_dimension=0,
        tiled=True,
    ).astype(jnp.float32)
    middle = x_res.astype(jnp.float32) + projected
    normed = middle * lax.rsqrt(jnp.mean(middle * middle, axis=-1, keepdims=True) + norm_eps)
    normed = (normed * gain_mid).astype(jnp.bfloat16)
    gathered = lax.all_gather(normed, "tp", axis=0, tiled=True)
    gate_pre = jnp.dot(gathered, whole_gate, preferred_element_type=jnp.float32)
    up_pre = jnp.dot(gathered, whole_up, preferred_element_type=jnp.float32)
    width = gate_pre.shape[1]
    joined = jnp.concatenate([gate_pre, up_pre], axis=1).astype(jnp.bfloat16)
    padded = extended(joined, (("sp", 0),), 1)
    taps = jnp.concatenate([conv_gate, conv_up], axis=1)
    mixed = padded[:-2] * taps[0] + padded[1:-1] * taps[1] + padded[2:] * taps[2]
    hidden = (jax.nn.silu(mixed[:, :width]) * mixed[:, width:]).astype(jnp.bfloat16)
    terms = jnp.dot(hidden, whole_down, preferred_element_type=jnp.float32)
    summed = lax.psum_scatter(
        terms.astype(jnp.bfloat16), "tp", scatter_dimension=0, tiled=True
    ).astype(jnp.float32)
    return (middle + summed).astype(jnp.bfloat16)


def solution(mesh):
    in_specs = (
        P(("sp", "tp"), None),
        P("sp", "tp"),
        P("sp", "tp"),
        P("sp", "tp"),
        P("sp", "tp"),
        P("sp", "tp"),
        P("sp", "tp"),
        P(),
        P(),
        P(),
        P(),
        P("tp", None),
        P("tp", None),
        P(),
        P("sp", "tp"),
        P("sp", "tp"),
        P(None, "tp"),
        P(None, "tp"),
        P("tp", "sp"),
    )
    out_specs = P(("sp", "tp"), None)
    body = functools.partial(on_device, mesh.shape["sp"], mesh.shape["tp"])
    return jax.shard_map(
        body, mesh=mesh, in_specs=in_specs, out_specs=out_specs, check_vma=False
    )
```
